32 devices in a mesh: grp: 2 (over y), fs: 4 (over z), tp: 4 (over x, core).
Axes of the slice: x: 2, y: 2, z: 4, core: 2. Of those that a mesh axis runs over, the one named last changes fastest.
Arguments:
- tokens: bfloat16 [6144, 2048], P(('grp', 'fs'), 'tp'), parts along dimension 0, may hold values from -6 to 6
- mix_gain: float32 [2048], replicated, may hold values from 0.1 to 1.9
- w_u: float32 [2048, 1024], P('fs', 'tp'), may hold values from -0.125 to 0.125
- w_v: float32 [2048, 1024], P('fs', 'tp'), may hold values from -0.125 to 0.125
- u_scale: float32 [1024], P('tp'), may hold values from 0.5 to 2
- v_scale: float32 [1024], P('tp'), may hold values from 0.5 to 2
- spatial: bfloat16 [8, 128, 128], P('tp'), may hold values from -0.5 to 0.5
- spatial_bias: float32 [8, 128], P('tp'), may hold values from 0.1 to 1.9
- w_mix: float32 [1024, 2048], P('tp', 'fs'), may hold values from -0.1875 to 0.1875
- mix_scale: float32 [1, 2048], P(None, 'fs'), may hold values from 0.5 to 2
- ffn_gain: float32 [2048], replicated, may hold values from 0.1 to 1.9
- w_gate: float32 [2048, 5632], P('fs', 'tp'), may hold values from -0.125 to 0.125
- w_up: float32 [2048, 5632], P('fs', 'tp'), may hold values from -0.125 to 0.125
- gate_scale: float32 [5632], P('tp'), may hold values from 0.5 to 2
- up_scale: float32 [5632], P('tp'), may hold values from 0.5 to 2
- w_down: float32 [5632, 2048], P('tp', 'fs'), may hold values from -0.078125 to 0.078125
- down_scale: float32 [1, 2048], P(None, 'fs'), may hold values from 0.5 to 2
Outputs:
- layer_out: bfloat16 [6144, 2048], P(('grp', 'fs'), 'tp'), parts along dimension 0
The draws below stay inside these ranges and needn't reach their ends.
There are 2 independent parts, one for each index of `grp`. The reference program is written for one: setup_inputs(seed, part) draws one part's arguments, and reference() takes and returns one part's arrays. A program takes and returns all parts, laid end to end along the dimension named above; an argument that names none is the same for every part. Nothing has to cross between parts.
All inputs are finite; a program needn't handle non-finite values.
Results may differ from the reference program's by a relative error of at most 0.024.
Values may be sent and summed in bfloat16 or wider, within the bound.
A program may use at most 128 MiB of HBM per device.

```python
import math
import jax
import jax.numpy as jnp
from jax import lax

D = 2048
SGD = 128
SG = 8
SW = 1024
FF = 5632
BLK = 128
TOKENS = 3072
N_TP = 4


def shard_levels(key, dims, shards, least, high):
    loudness = 1.0
    for position, shards_of in shards:
        steps = jax.random.uniform(jax.random.fold_in(jax.random.fold_in(key, 6), position), (shards_of,), jnp.float32, least / len(shards), high / len(shards))
        loudness = loudness * jnp.repeat(jnp.exp(steps), dims[position] // shards_of).reshape((-1,) + (1,) * (len(dims) - 1 - position))
    return loudness


def centred(rng, shape, scale, limit, cuts=(), dtype=jnp.bfloat16):
    drawn = scale * jax.random.normal(rng, shape, jnp.float32)
    if cuts:
        drawn = drawn * shard_levels(rng, shape, cuts, -0.22, 0.18)
    return jnp.clip(drawn, -limit, limit).astype(dtype)


def setup_inputs(seed: int = 0, part: int = 0) -> dict:
    splits = jax.random.split(jax.random.key(seed), 18)
    part_keys = jax.random.split(jax.random.fold_in(splits[17], part), 18)
    return {
        "tokens": centred(part_keys[0], (TOKENS, D), 1.0, 6.0, ((0, 4), (1, 4))),
        "mix_gain": jnp.clip(1.0 + 0.18 * jax.random.normal(splits[1], (D,), jnp.float32), 0.1, 1.9),
        "w_u": centred(splits[2], (D, SW), D ** -0.5, 0.125, ((0, 4), (1, 4)), jnp.float32),
        "w_v": centred(splits[3], (D, SW), D ** -0.5, 0.125, ((0, 4), (1, 4)), jnp.float32),
        "u_scale": jnp.clip(jnp.exp(math.log(2.0) - 1.3862944 * jax.random.uniform(splits[4], (SW,), jnp.float32) ** shard_levels(splits[4], (SW,), ((0, 4),), -0.2, 0.2)), 0.5, 2.0),
        "v_scale": jnp.clip(jnp.exp(math.log(2.0) - 1.3862944 * jax.random.uniform(splits[5], (SW,), jnp.float32) ** shard_levels(splits[5], (SW,), ((0, 4),), -0.2, 0.2)), 0.5, 2.0),
        "spatial": centred(splits[6], (SG, BLK, BLK), BLK ** -0.5, 0.5, ((0, 4),)),
        "spatial_bias": jnp.clip(1.0 + 0.18 * jax.random.normal(splits[7], (SG, BLK), jnp.float32), 0.1, 1.9),
        "w_mix": centred(splits[8], (SW, D), SW ** -0.5, 0.1875, ((0, 4), (1, 4)), jnp.float32),
        "mix_scale": jnp.clip(jnp.exp(math.log(2.0) - 1.3862944 * jax.random.uniform(splits[9], (1, D), jnp.float32) ** shard_levels(splits[9], (1, D), ((1, 4),), -0.2, 0.2)), 0.5, 2.0),
        "ffn_gain": jnp.clip(1.0 + 0.18 * jax.random.normal(splits[10], (D,), jnp.float32), 0.1, 1.9),
        "w_gate": centred(splits[11], (D, FF), D ** -0.5, 0.125, ((0, 4), (1, 4)), jnp.float32),
        "w_up": centred(splits[12], (D, FF), D ** -0.5, 0.125, ((0, 4), (1, 4)), jnp.float32),
        "gate_scale": jnp.clip(jnp.exp(math.log(2.0) - 1.3862944 * jax.random.uniform(splits[13], (FF,), jnp.float32) ** shard_levels(splits[13], (FF,), ((0, 4),), -0.2, 0.2)), 0.5, 2.0),
        "up_scale": jnp.clip(jnp.exp(math.log(2.0) - 1.3862944 * jax.random.uniform(splits[14], (FF,), jnp.float32) ** shard_levels(splits[14], (FF,), ((0, 4),), -0.2, 0.2)), 0.5, 2.0),
        "w_down": centred(splits[15], (FF, D), FF ** -0.5, 0.078125, ((0, 4), (1, 4)), jnp.float32),
        "down_scale": jnp.clip(jnp.exp(math.log(2.0) - 1.3862944 * jax.random.uniform(splits[16], (1, D), jnp.float32) ** shard_levels(splits[16], (1, D), ((1, 4),), -0.2, 0.2)), 0.5, 2.0),
    }


eps = 1e-06

def norm_rows(rows, gain):
    wide = rows.astype(jnp.float32)
    factor = lax.rsqrt(lax.optimization_barrier(jnp.mean(wide * wide, axis=1, keepdims=True)) + eps)
    return (wide * factor * gain).astype(jnp.bfloat16)

def sliced_sum(hidden, weight, scale):
    width = hidden.shape[1] // N_TP
    total = jnp.zeros((hidden.shape[0], weight.shape[1]), jnp.float32)
    weight_half = weight.astype(jnp.bfloat16)
    for index in range(N_TP):
        left = hidden[:, index * width:(index + 1) * width]
        right = weight_half[index * width:(index + 1) * width]
        term = jnp.dot(left, right, preferred_element_type=jnp.float32) * scale
        rounded = lax.optimization_barrier(term.astype(jnp.bfloat16))
        total = total + rounded.astype(jnp.float32)
    return total

def reference(tokens, mix_gain, w_u, w_v, u_scale, v_scale, spatial, spatial_bias, w_mix, mix_scale, ffn_gain, w_gate, w_up, gate_scale, up_scale, w_down, down_scale):
    normed_in = norm_rows(tokens, mix_gain)
    u_act = jax.nn.gelu(jnp.dot(normed_in, w_u.astype(jnp.bfloat16), preferred_element_type=jnp.float32) * u_scale, approximate=False)
    v_act = jax.nn.gelu(jnp.dot(normed_in, w_v.astype(jnp.bfloat16), preferred_element_type=jnp.float32) * v_scale, approximate=False).astype(jnp.bfloat16)
    count = tokens.shape[0]
    blocks = v_act.reshape(count // BLK, BLK, SG, SGD).astype(jnp.float32)
    causal = jnp.arange(BLK)[:, None] >= jnp.arange(BLK)[None, :]
    masked = jnp.where(causal[None], spatial.astype(jnp.float32), jnp.float32(0.0))
    spatial_out = jnp.einsum('gts,nsgc->ntgc', masked, blocks) + spatial_bias.T[None, :, :, None]
    gated = (u_act * spatial_out.reshape(count, SW)).astype(jnp.bfloat16)
    mixed = sliced_sum(gated, w_mix, mix_scale)
    resid = (tokens.astype(jnp.float32) + mixed).astype(jnp.bfloat16)
    normed_ffn = norm_rows(resid, ffn_gain)
    gate_val = jnp.dot(normed_ffn, w_gate.astype(jnp.bfloat16), preferred_element_type=jnp.float32) * gate_scale
    up_val = jnp.dot(normed_ffn, w_up.astype(jnp.bfloat16), preferred_element_type=jnp.float32) * up_scale
    act = (jax.nn.silu(gate_val) * up_val).astype(jnp.bfloat16)
    down_sum = sliced_sum(act, w_down, down_scale)
    return (resid.astype(jnp.float32) + down_sum).astype(jnp.bfloat16)
```

```python
import functools

import jax
import jax.numpy as jnp
from jax import lax
from jax.experimental import pallas as pl
from jax.experimental.pallas import tpu as pltpu
from jax.sharding import PartitionSpec as P

MESH = pl.DeviceIdType.MESH
eps = 1e-06
H = 2
C = 4
half_root = 0.7071067811865476
f32 = jnp.float32
bf16 = jnp.bfloat16


def gelu(a):
    return 0.5 * a * (1.0 + lax.erf(a * half_root))


def up_to(a, b):
    return -(-a // b) * b


def layer_kernel(
    dims,
    tokens,
    mix_gain,
    ffn_gain,
    w_u,
    w_v,
    w_mix,
    w_gate,
    w_up,
    w_down,
    u_scale,
    v_scale,
    spatial,
    bias,
    mix_scale,
    gate_scale,
    up_scale,
    down_scale,
    out,
    uv_stage,
    mix_stage,
    gate_stage,
    up_stage,
    uv_buf,
    mix_buf,
    gate_buf,
    up_buf,
    down_buf,
    tok_buf,
    res_buf,
    gated,
    silu_buf,
    act,
    give_buf,
    pair_buf,
    keep,
    send_buf,
    far_buf,
    load_sem,
    z_send,
    z_recv,
    y_send,
    y_recv,
    a_send,
    a_fwd,
    a_recv,
    gx_send,
    gz_send,
    gd_send,
    gfz_send,
    gfx_send,
    g_recv,
    p_send,
    p_recv,
    m_send,
    m_recv,
    f_send,
    f_recv,
):
    n, n_tp, parts = dims
    nx = n_tp // 2
    i = lax.axis_index("fs")
    g = lax.axis_index("grp")
    t = lax.axis_index("tp")
    x, c = t // 2, t % 2
    m = i % 2
    rows, dt = tokens.shape
    dr, ff = w_gate.shape
    df = w_down.shape[1]
    per = dt // df
    rt = rows // H
    ct = rows // C
    wide = gate_buf.shape[2]
    rest = ff - wide
    padded = up_to(rest, 128)
    widths = (wide, padded)
    heights = (wide, rest)
    partner = {"tp": x * 2 + 1 - c}
    across = {"grp": 1 - g}
    beside = {"fs": i + 1 - 2 * m}

    def far(k):
        return lax.rem(x + k, nx)

    def far_id(k):
        return {"tp": far(k) * 2 + c}

    def remote(src, dst, ss, rs, device):
        return pltpu.make_async_remote_copy(
            src_ref=src,
            dst_ref=dst,
            send_sem=ss,
            recv_sem=rs,
            device_id=device,
            device_id_type=MESH,
        )

    width = w_u.shape[1]
    loads = [
        pltpu.make_async_copy(w_u, uv_stage.at[0], load_sem.at[0]),
        pltpu.make_async_copy(w_v, uv_stage.at[1], load_sem.at[1]),
        pltpu.make_async_copy(w_mix, mix_stage, load_sem.at[2]),
        pltpu.make_async_copy(w_gate, gate_stage, load_sem.at[3]),
        pltpu.make_async_copy(w_up, up_stage, load_sem.at[4]),
        pltpu.make_async_copy(w_down, silu_buf.at[pl.ds(0, ff), pl.ds(0, df)], load_sem.at[5]),
        pltpu.make_async_copy(tokens, tok_buf.at[t], load_sem.at[6]),
    ]
    for copy in loads:
        copy.start()

    barrier = pltpu.get_barrier_semaphore()
    for k in range(1, n):
        pl.semaphore_signal(barrier, 1, device_id={"fs": (i + k) % n}, device_id_type=MESH)
    pl.semaphore_signal(barrier, 1, device_id=across, device_id_type=MESH)
    pl.semaphore_signal(barrier, 1, device_id=partner, device_id_type=MESH)
    for k in range(1, nx):
        pl.semaphore_signal(barrier, 1, device_id=far_id(k), device_id_type=MESH)
    pl.semaphore_wait(barrier, (n - 1) + 2 + (nx - 1))

    UV, MIX, GATE, UP, DOWN = range(5)
    bufs = (uv_buf, mix_buf, gate_buf, up_buf) + (down_buf,) * parts
    streams = len(bufs)
    dc = df // parts

    def view(k, slot, who, h):
        ref = bufs[k]
        if k < GATE:
            count = ref.shape[1] // 2
            return ref.at[slot, pl.ds(pl.multiple_of(who * count, 16), count), :]
        if k < DOWN:
            count = dr // 2
            sl = pl.ds(pl.multiple_of(who * count, 16), count)
            return ref.at[slot, sl, pl.ds(0, widths[h])]
        count = heights[h] // 2
        sl = pl.ds(pl.multiple_of(who * count, 16), count)
        return ref.at[slot, sl, pl.ds((k - DOWN) * dc, dc)]

    def z_copy(k, src, dst, step, h, sem):
        return remote(
            view(k, src, g, h),
            view(k, dst, g, h),
            z_send.at[k, sem],
            z_recv.at[k, dst],
            {"fs": jnp.clip(i + step, 0, n - 1)},
        )

    def y_copy(k, j, who, h):
        ref = view(k, j, who, h)
        return remote(ref, ref, y_send.at[k, j], y_recv.at[k, j], across)

    def by_half(k, f):
        if k < GATE:
            f(0)
            return
        for h in range(2):

            @pl.when(m == h)
            def _():
                f(h)

    def own_each(k, act_on):
        stride = 1 if k < GATE else 2

        def each(h):
            if k >= GATE:

                @pl.when(i + 1 < n)
                def _():
                    act_on(z_copy(k, n, i, 1, 1 - h, n + 2))

                @pl.when(i > 0)
                def _():
                    act_on(z_copy(k, n, i, -1, 1 - h, n + 3))

            @pl.when(i + stride < n)
            def _():
                act_on(z_copy(k, i, i, stride, h, n))

            @pl.when(i - stride >= 0)
            def _():
                act_on(z_copy(k, i, i, -stride, h, n + 1))

        by_half(k, each)

    def own(k):
        own_each(k, lambda copy: copy.start())

    def service(k, s):
        if s >= n:
            return
        stride = 1 if k < GATE else 2

        def each(h):
            left, right = i - s, i + s

            @pl.when(left >= 0)
            def _():
                z_copy(k, left, left, stride, h, left).wait_recv()

                @pl.when(i + stride < n)
                def _():
                    z_copy(k, left, left, stride, h, left).start()

                y_copy(k, left, g, h).start()

            @pl.when(right < n)
            def _():
                z_copy(k, right, right, -stride, h, right).wait_recv()

                @pl.when(i - stride >= 0)
                def _():
                    z_copy(k, right, right, -stride, h, right).start()

                y_copy(k, right, g, h).start()

        by_half(k, each)

    def run(k, begin, end):
        for s in range(begin, end):
            service(k, s)

    def finish(k):
        def each(h):
            for s in range(1, n):
                y_copy(k, lax.rem(i + s, n), 1 - g, h).wait_recv()

        by_half(k, each)

    def drain(k):
        stride = 1 if k < GATE else 2
        own_each(k, lambda copy: copy.wait_send())

        def each(h):
            for s in range(1, n):
                j = lax.rem(i + s, n)
                y_copy(k, j, g, h).wait_send()

                @pl.when(jnp.logical_and(j < i, i + stride < n))
                def _():
                    z_copy(k, j, j, stride, h, j).wait_send()

                @pl.when(jnp.logical_and(j > i, i - stride >= 0))
                def _():
                    z_copy(k, j, j, -stride, h, j).wait_send()

        by_half(k, each)

    def chunk(h):
        return pl.ds(h * rt, rt)

    def ag_x(k, h):
        return remote(
            tokens.at[chunk(h), :],
            tok_buf.at[t, chunk(h), :],
            a_send.at[k, h],
            a_recv.at[t, h],
            far_id(k) if k else partner,
        )

    def ag_fwd(k, h):
        slot = far(k) * 2 + c
        ref = tok_buf.at[slot, chunk(h), :]
        return remote(ref, ref, a_fwd.at[k, h], a_recv.at[slot, h], partner)

    def ag_in(k, h):
        slot = far(k) * 2 + 1 - c
        ref = tok_buf.at[slot, chunk(h), :]
        return remote(ref, ref, a_fwd.at[0, h], a_recv.at[slot, h], partner)

    def rchunk(q):
        return pl.ds(q * ct, ct)

    def block(e, slot, q):
        return res_buf.at[e, slot, rchunk(q), :]

    def gx(k, q):
        return remote(block(0, t, q), block(0, t, q), gx_send.at[k, q], g_recv.at[0, t, q], far_id(k))

    def gz(q):
        return remote(block(0, t, q), block(1, t, q), gz_send.at[q], g_recv.at[1, t, q], beside)

    def gd(e, k, q):
        slot = far(k) * 2 + c
        ref = block(e, slot, q)
        return remote(ref, ref, gd_send.at[e, k, q], g_recv.at[e, slot, q], partner)

    def gd_in(e, k, q):
        slot = far(k) * 2 + 1 - c
        ref = block(e, slot, q)
        return remote(ref, ref, gd_send.at[e, k, q], g_recv.at[e, slot, q], partner)

    def gfz(k, q):
        slot = far(k) * 2 + c
        return remote(
            block(0, slot, q), block(1, slot, q), gfz_send.at[k, q], g_recv.at[1, slot, q], beside
        )

    def gfx(k, q):
        return remote(block(1, t, q), block(1, t, q), gfx_send.at[k, q], g_recv.at[1, t, q], far_id(k))

    def g_start(q):
        for k in range(1, nx):
            gx(k, q).start()
        gz(q).start()
        gd(0, 0, q).start()

    def g_first(q):
        for k in range(1, nx):
            gd(0, k, q).wait_recv()
            if q < C // 2:
                gfz(k, q).start()
            gd(0, k, q).start()
        gd(1, 0, q).wait_recv()
        if q >= C // 2:
            for k in range(1, nx):
                gfx(k, q).start()
        gd(1, 0, q).start()

    def g_second(q):
        for k in range(1, nx):
            gd(1, k, q).wait_recv()
            gd(1, k, q).start()

    def g_ready(e, q):
        for k in range(nx):
            gd_in(e, k, q).wait_recv()

    def g_drain():
        for q in range(C):
            gz(q).wait_send()
            for e in range(2):
                for k in range(nx):
                    gd(e, k, q).wait_send()
            for k in range(1, nx):
                gx(k, q).wait_send()
                if q < C // 2:
                    gfz(k, q).wait_send()
                else:
                    gfx(k, q).wait_send()

    bw = dt // parts

    def weight(buf, owner, p):
        ws = [buf[owner * per + q, :, p * dc : (p + 1) * dc] for q in range(per)]
        return ws[0] if per == 1 else jnp.concatenate(ws, axis=1)

    def pair_copy(r, p, xo, e, h):
        return remote(
            give_buf.at[p, xo, e, h],
            pair_buf.at[p, xo, e, h],
            p_send.at[r, p, xo, e, h],
            p_recv.at[r, p, xo, e, h],
            partner,
        )

    def partials(r, p, xo, e, h, left, buf):
        give_buf[p, xo, e, h] = jnp.dot(
            left, weight(buf, xo * 2 + 1 - c, p), preferred_element_type=f32
        ).astype(bf16)
        pair_copy(r, p, xo, e, h).start()
        keep[p, xo, e, h] = jnp.dot(left, weight(buf, xo * 2 + c, p), preferred_element_type=f32)

    def both(r, p, xo, e, h):
        pair_copy(r, p, xo, e, h).wait_recv()
        return keep[p, xo, e, h] + pair_buf[p, xo, e, h].astype(f32)

    def mix_copy(p, k, h, slot):
        xo = far(k)
        return remote(
            send_buf.at[p, xo, 0, h],
            far_buf.at[p, slot, 0, h],
            m_send.at[p, xo, h],
            m_recv.at[p, slot, h],
            far_id(k),
        )

    def far_copy(p, src, dst, device):
        return remote(
            send_buf.at[(p,) + src],
            far_buf.at[(p,) + dst],
            f_send.at[(p,) + src],
            f_recv.at[(p,) + dst],
            device,
        )

    def x_one(p, k, e):
        return far_copy(p, (far(k), e, 0), (x, e, 0), far_id(k))

    def x_one_in(p, k, e):
        return far_copy(p, (far(k), e, 0), (far(k), e, 0), far_id(k))

    def z_one(p, k):
        return far_copy(p, (far(k), 1, 1), (far(k), 0, 1), beside)

    def z_two(p):
        return far_copy(p, (x, 1, 0), (x, 0, 0), beside)

    def x_two(p, k):
        return far_copy(p, (far(k), 0, 1), (x, 1, 1), far_id(k))

    def x_two_in(p, k):
        return far_copy(p, (far(k), 0, 1), (far(k), 1, 1), far_id(k))

    def arrived(p, a, e, h):
        return far_buf[p, a, e, h].astype(f32)

    def factor(rows_in):
        total = jnp.zeros((rows_in.shape[0], 1), f32)
        for q in range(n_tp):
            part = rows_in[:, q * dt : (q + 1) * dt].astype(f32)
            total = total + jnp.sum(part * part, axis=1, keepdims=True)
        return lax.rsqrt(total / (n_tp * dt) + eps)

    def column(gain, s):
        lanes = gain[0:1, pl.ds(pl.multiple_of(i * dr + s * 128, 128), 128)]
        return jnp.broadcast_to(lanes, (128, 128)).T[:, :1]

    for h in range(H):
        for k in list(range(1, nx)) + [0]:
            ag_x(k, h).start()
    loads[0].wait()
    loads[1].wait()
    for s in range(dr // 128):
        sl = slice(s * 128, (s + 1) * 128)
        gain = column(mix_gain, s)
        uv_buf[i, sl, :width] = (uv_stage[0, sl, :] * gain * u_scale[0:1, :]).astype(bf16)
        uv_buf[i, sl, width:] = (uv_stage[1, sl, :] * gain * v_scale[0:1, :]).astype(bf16)
    own(UV)
    loads[2].wait()
    mix_buf[i] = (mix_stage[...] * mix_scale[0:1, :]).astype(bf16)
    own(MIX)

    def cast_in(stage, scale, buf):
        for s in range(dr // 128):
            sl = slice(s * 128, (s + 1) * 128)
            gain = column(ffn_gain, s)
            for h, (lo, hi) in enumerate(((0, wide), (wide, ff))):
                slot = jnp.where(m == h, i, n)
                buf[slot, sl, : hi - lo] = (
                    stage[sl, lo:hi] * gain * scale[0:1, lo:hi]
                ).astype(bf16)
                if hi - lo < widths[h]:
                    buf[slot, sl, hi - lo : widths[h]] = jnp.zeros(
                        (128, widths[h] - hi + lo), bf16
                    )

    loads[3].wait()
    cast_in(gate_stage, gate_scale, gate_buf)
    loads[4].wait()
    cast_in(up_stage, up_scale, up_buf)
    loads[5].wait()
    for h, (lo, hi) in enumerate(((0, wide), (wide, ff))):
        slot = jnp.where(m == h, i, n)
        down_buf[slot, : hi - lo, :] = (silu_buf[lo:hi, :df] * down_scale[0:1, :]).astype(bf16)

    @pl.when(m == 1)
    def _():
        for j in range(n):
            if padded < wide:
                gate_buf[j, :, padded:] = jnp.zeros((dr, wide - padded), bf16)
                up_buf[j, :, padded:] = jnp.zeros((dr, wide - padded), bf16)
            down_buf[j, rest:, :] = jnp.zeros((wide - rest, df), bf16)

    for s in range(1, n):
        service(UV, s)
        service(MIX, s)
        if s == max(n - 2, 1):
            own(GATE)
    for h in range(H):
        for k in range(1, nx):
            ag_fwd(k, h).wait_recv()
            ag_fwd(k, h).start()
    for h in range(H):
        for k in range(nx):
            ag_in(k, h).wait_recv()
    loads[6].wait()
    finish(UV)

    groups, span = spatial.shape[0], spatial.shape[1]
    lanes = width // groups
    causal = lax.broadcasted_iota(jnp.int32, (span, span), 0) >= lax.broadcasted_iota(
        jnp.int32, (span, span), 1
    )
    tilt = [jnp.broadcast_to(bias[q : q + 1, :], (span, span)).T[:, :1] for q in range(groups)]

    def gather_rows(pieces):
        return jnp.concatenate(pieces, axis=1)

    for h in range(H):
        left = gather_rows([tok_buf[q, chunk(h), :] for q in range(n_tp)])
        pre = jnp.dot(left, uv_buf[...].reshape(-1, 2 * width), preferred_element_type=f32)
        pre = pre * factor(left)
        u = gelu(pre[:, :width])
        v = gelu(pre[:, width:]).astype(bf16)
        for q in range(groups):
            mat = jnp.where(causal, spatial[q].astype(f32), 0.0).astype(bf16)
            cols = slice(q * lanes, (q + 1) * lanes)
            for b in range(rt // span):
                sl = slice(b * span, (b + 1) * span)
                mixed = jnp.dot(mat, v[sl, cols], preferred_element_type=f32) + tilt[q]
                gated[h * rt + b * span : h * rt + (b + 1) * span, cols] = (
                    u[sl, cols] * mixed
                ).astype(bf16)
    finish(MIX)

    for k in range(1, nx):
        for h in range(H):
            for p in range(parts):
                partials(0, p, far(k), 0, h, gated[chunk(h), :], mix_buf)
        for h in range(H):
            for p in range(parts):
                send_buf[p, far(k), 0, h] = both(0, p, far(k), 0, h).astype(bf16)
                mix_copy(p, k, h, x).start()
    service(GATE, 1)
    own(UP)
    for h in range(H):
        for p in range(parts):
            partials(0, p, x, 0, h, gated[chunk(h), :], mix_buf)
    service(GATE, 2)
    for h in range(H):
        for p in range(parts):
            total = both(0, p, x, 0, h)
            for k in range(1, nx):
                mix_copy(p, k, h, far(k)).wait_recv()
                total = total + arrived(p, far(k), 0, h)
            cols = slice(p * bw, (p + 1) * bw)
            res_buf[0, t, chunk(h), cols] = (
                tok_buf[t, chunk(h), cols].astype(f32) + total
            ).astype(bf16)
        for q in range(h * (C // H), (h + 1) * (C // H)):
            g_start(q)
    run(GATE, 3, n)
    service(UP, 1)
    g_first(0)
    g_first(1)
    service(UP, 2)
    for k in range(parts):
        own(DOWN + k)
    g_first(2)
    g_first(3)
    finish(GATE)

    def gate_tiles(e, begin, end):
        def body(b, carry):
            sl = pl.ds(pl.multiple_of(b * ct, 64), ct)
            left = gather_rows([res_buf[e, q, sl, :] for q in range(n_tp)])
            inv = factor(left)
            a = jnp.dot(left, gate_buf[:n].reshape(-1, wide), preferred_element_type=f32) * inv
            silu_buf[pl.ds(pl.multiple_of(e * rows + b * ct, 64), ct), :] = (
                a / (1.0 + jnp.exp(-a)) * inv
            )
            return carry

        lax.fori_loop(begin, end, body, 0)

    def up_tiles(e):
        def body(b, carry):
            sl = pl.ds(pl.multiple_of(b * ct, 64), ct)
            flat = pl.ds(pl.multiple_of(e * rows + b * ct, 64), ct)
            left = gather_rows([res_buf[e, q, sl, :] for q in range(n_tp)])
            a = jnp.dot(left, up_buf[:n].reshape(-1, wide), preferred_element_type=f32)
            act[flat, :] = (silu_buf[flat, :] * a).astype(bf16)
            return carry

        lax.fori_loop(0, C, body, 0)

    for q in range(C):
        g_ready(0, q)
    g_second(0)
    g_second(1)
    gate_tiles(0, 0, C)
    g_second(2)
    g_second(3)
    run(UP, 3, n)
    for q in range(C):
        g_ready(1, q)
    gate_tiles(1, 0, C)
    service(DOWN, 1)
    finish(UP)
    up_tiles(0)
    run(DOWN, 2, 3)
    up_tiles(1)
    for p in range(1, parts):
        service(DOWN + p, 1)
    run(DOWN, 3, n)
    for p in range(1, parts):
        service(DOWN + p, 2)

    for p in range(parts):
        for k in range(1, nx + 1):
            for h in range(H):
                pair_copy(0, p, far(k), 0, h).wait_send()
                if k < nx:
                    mix_copy(p, k, h, x).wait_send()

    def sum_first(p):
        for e in (1, 0):
            for k in range(1, nx + 1):
                for h in range(H):
                    left = act[e * rows + h * rt : e * rows + (h + 1) * rt, :]
                    partials(1, p, far(k), e, h, left, down_buf)
        for e in (1, 0):
            for k in range(1, nx + 1):
                xo = far(k)
                for h in range(H):
                    value = both(1, p, xo, e, h)
                    if h == 0 and k < nx:
                        send_buf[p, xo, e, 0] = value.astype(bf16)
                        x_one(p, k, e).start()
                    elif h == 1 and e == 1:
                        send_buf[p, xo, 1, 1] = value.astype(bf16)
                        z_one(p, k).start()
                    else:
                        keep[p, xo, e, h] = value

    def sum_second(p):
        for k in range(1, nx):
            z_in = z_one(p, k)
            z_in.wait_recv()
            send_buf[p, far(k), 0, 1] = (
                keep[p, far(k), 0, 1] + arrived(p, far(k), 0, 1)
            ).astype(bf16)
            x_two(p, k).start()
        value = keep[p, x, 1, 0]
        for k in range(1, nx):
            x_one_in(p, k, 1).wait_recv()
            value = value + arrived(p, far(k), 1, 0)
        send_buf[p, x, 1, 0] = value.astype(bf16)
        z_two(p).start()

    def sum_last(p):
        cols = slice(p * bw, (p + 1) * bw)
        total = keep[p, x, 0, 0]
        for k in range(1, nx):
            x_one_in(p, k, 0).wait_recv()
            total = total + arrived(p, far(k), 0, 0)
        z_two(p).wait_recv()
        total = total + arrived(p, x, 0, 0)
        out[chunk(0), cols] = (res_buf[0, t, chunk(0), cols].astype(f32) + total).astype(bf16)
        z_one(p, nx).wait_recv()
        total = keep[p, x, 0, 1] + arrived(p, x, 0, 1)
        for k in range(1, nx):
            x_two_in(p, k).wait_recv()
            total = total + arrived(p, far(k), 1, 1)
        out[chunk(1), cols] = (res_buf[0, t, chunk(1), cols].astype(f32) + total).astype(bf16)

    def sum_drain(p):
        for k in range(1, nx + 1):
            z_one(p, k).wait_send()
            for e in range(2):
                for h in range(H):
                    pair_copy(1, p, far(k), e, h).wait_send()
                if k < nx:
                    x_one(p, k, e).wait_send()
            if k < nx:
                x_two(p, k).wait_send()
        z_two(p).wait_send()

    finish(DOWN)
    sum_first(0)
    for p in range(1, parts):
        run(DOWN + p, 3, n)
        sum_second(p - 1)
        finish(DOWN + p)
        sum_first(p)
        sum_last(p - 1)
    sum_second(parts - 1)
    sum_last(parts - 1)

    for p in range(parts):
        sum_drain(p)
    for h in range(H):
        for k in range(nx):
            ag_x(k, h).wait_send()
        for k in range(1, nx):
            ag_fwd(k, h).wait_send()
    g_drain()
    for k in range(streams):
        drain(k)


def local(
    dims,
    tokens,
    mix_gain,
    w_u,
    w_v,
    u_scale,
    v_scale,
    spatial,
    spatial_bias,
    w_mix,
    mix_scale,
    ffn_gain,
    w_gate,
    w_up,
    gate_scale,
    up_scale,
    w_down,
    down_scale,
):
    n, n_tp = dims
    nx = n_tp // 2
    rows, dt = tokens.shape
    dr, ff = w_gate.shape
    df = mix_scale.shape[1]
    parts = 2 if df % 256 == 0 else 1
    streams = 4 + parts
    wide = up_to(-(-ff // 2), 128)
    rt, bw = rows // H, dt // parts
    hbm = pl.BlockSpec(memory_space=pl.ANY)
    vmem = pl.BlockSpec(memory_space=pltpu.VMEM)
    dma = pltpu.SemaphoreType.DMA
    sums = (parts, nx, 2, H, rt, bw)
    return pl.pallas_call(
        functools.partial(layer_kernel, (n, n_tp, parts)),
        out_shape=jax.ShapeDtypeStruct((rows, dt), bf16),
        in_specs=[hbm, vmem, vmem] + [hbm] * 6 + [vmem] * 8,
        out_specs=vmem,
        scratch_shapes=[
            pltpu.VMEM((2,) + w_u.shape, f32),
            pltpu.VMEM(w_mix.shape, f32),
            pltpu.VMEM(w_gate.shape, f32),
            pltpu.VMEM(w_up.shape, f32),
            pltpu.VMEM((n, dr, 2 * w_u.shape[1]), bf16),
            pltpu.VMEM((n,) + w_mix.shape, bf16),
            pltpu.VMEM((n + 1, dr, wide), bf16),
            pltpu.VMEM((n + 1, dr, wide), bf16),
            pltpu.VMEM((n + 1, wide, df), bf16),
            pltpu.VMEM((n_tp, rows, dt), bf16),
            pltpu.VMEM((2, n_tp, rows, dt), bf16),
            pltpu.VMEM((rows, w_u.shape[1]), bf16),
            pltpu.VMEM((2 * rows, wide), f32),
            pltpu.VMEM((2 * rows, wide), bf16),
            pltpu.VMEM(sums, bf16),
            pltpu.VMEM(sums, bf16),
            pltpu.VMEM(sums, f32),
            pltpu.VMEM(sums, bf16),
            pltpu.VMEM(sums, bf16),
            dma((7,)),
            dma((streams, n + 4)),
            dma((streams, n)),
            dma((streams, n)),
            dma((streams, n)),
            dma((nx, H)),
            dma((nx, H)),
            dma((n_tp, H)),
            dma((nx, C)),
            dma((C,)),
            dma((2, nx, C)),
            dma((nx, C)),
            dma((nx, C)),
            dma((2, n_tp, C)),
            dma((2, parts, nx, 2, H)),
            dma((2, parts, nx, 2, H)),
            dma((parts, nx, H)),
            dma((parts, nx, H)),
            dma((parts, nx, 2, H)),
            dma((parts, nx, 2, H)),
        ],
        compiler_params=pltpu.CompilerParams(
            collective_id=0, has_side_effects=True, vmem_limit_bytes=67000000
        ),
    )(
        tokens,
        mix_gain.reshape(1, -1),
        ffn_gain.reshape(1, -1),
        w_u,
        w_v,
        w_mix,
        w_gate,
        w_up,
        w_down,
        u_scale.reshape(1, -1),
        v_scale.reshape(1, -1),
        spatial,
        spatial_bias,
        mix_scale,
        gate_scale.reshape(1, -1),
        up_scale.reshape(1, -1),
        down_scale,
    )


def solution(mesh):
    placed = (
        P(("grp", "fs"), "tp"),
        P(),
        P("fs", "tp"),
        P("fs", "tp"),
        P("tp"),
        P("tp"),
        P("tp", None, None),
        P("tp", None),
        P("tp", "fs"),
        P(None, "fs"),
        P(),
        P("fs", "tp"),
        P("fs", "tp"),
        P("tp"),
        P("tp"),
        P("tp", "fs"),
        P(None, "fs"),
    )
    dims = (mesh.shape["fs"], mesh.shape["tp"])
    return jax.shard_map(
        functools.partial(local, dims),
        mesh=mesh,
        in_specs=placed,
        out_specs=P(("grp", "fs"), "tp"),
        check_vma=False,
    )
```

```python
import functools

import jax
import jax.numpy as jnp
from jax import lax
from jax.experimental import pallas as pl
from jax.experimental.pallas import tpu as pltpu
from jax.sharding import PartitionSpec as P

MESH = pl.DeviceIdType.MESH
eps = 1e-06
H = 2
C = 4
DIAG = 0
GSUB = 2
USUB = 4
half_root = 0.7071067811865476
f32 = jnp.float32
bf16 = jnp.bfloat16


def gelu(a):
    return 0.5 * a * (1.0 + lax.erf(a * half_root))


def up_to(a, b):
    return -(-a // b) * b


def layer_kernel(
    dims,
    tokens,
    mix_gain,
    ffn_gain,
    w_u,
    w_v,
    w_mix,
    w_gate,
    w_up,
    w_down,
    u_scale,
    v_scale,
    spatial,
    bias,
    mix_scale,
    gate_scale,
    up_scale,
    down_scale,
    out,
    uv_stage,
    mix_stage,
    gate_stage,
    up_stage,
    u_buf,
    v_buf,
    mix_buf,
    gate_buf,
    up_buf,
    down_buf,
    tok_buf,
    res_buf,
    gated,
    silu_buf,
    act,
    give_buf,
    pair_buf,
    keep,
    send_buf,
    far_buf,
    load_sem,
    z_send,
    z_recv,
    y_send,
    y_recv,
    a_send,
    a_fwd,
    a_recv,
    gx_send,
    gz_send,
    gd_send,
    gfz_send,
    gfx_send,
    g_recv,
    p_send,
    p_recv,
    f_send,
    f_recv,
):
    n, n_tp, parts = dims
    nx = n_tp // 2
    i = lax.axis_index("fs")
    g = lax.axis_index("grp")
    t = lax.axis_index("tp")
    x, c = t // 2, t % 2
    quad = i % 4
    odd = i % 2
    m = jnp.where(jnp.logical_or(quad == 0, quad == 3), 1, 0)
    rows, dt = tokens.shape
    dr, ff = w_gate.shape
    df = w_down.shape[1]
    per = dt // df
    rt = rows // H
    ct = rows // C
    wide = gate_buf.shape[2]
    rest = ff - wide
    padded = up_to(rest, 128)
    widths = (wide, padded)
    heights = (wide, rest)
    partner = {"tp": x * 2 + 1 - c}
    across = {"grp": 1 - g}
    beside = {"fs": i + 1 - 2 * odd}

    def far(k):
        return lax.rem(x + k, nx)

    def far_id(k):
        return {"tp": far(k) * 2 + c}

    def remote(src, dst, ss, rs, device):
        return pltpu.make_async_remote_copy(
            src_ref=src,
            dst_ref=dst,
            send_sem=ss,
            recv_sem=rs,
            device_id=device,
            device_id_type=MESH,
        )

    width = w_u.shape[1]
    loads = [
        pltpu.make_async_copy(w_u, uv_stage.at[0], load_sem.at[0]),
        pltpu.make_async_copy(w_v, uv_stage.at[1], load_sem.at[1]),
        pltpu.make_async_copy(w_mix, mix_stage, load_sem.at[2]),
        pltpu.make_async_copy(w_gate, gate_stage, load_sem.at[3]),
        pltpu.make_async_copy(w_up, up_stage, load_sem.at[4]),
        pltpu.make_async_copy(w_down, silu_buf.at[pl.ds(0, ff), pl.ds(0, df)], load_sem.at[5]),
        pltpu.make_async_copy(tokens, tok_buf.at[t], load_sem.at[6]),
    ]
    for copy in loads:
        copy.start()

    barrier = pltpu.get_barrier_semaphore()
    for k in range(1, n):
        pl.semaphore_signal(barrier, 1, device_id={"fs": (i + k) % n}, device_id_type=MESH)
    pl.semaphore_signal(barrier, 1, device_id=across, device_id_type=MESH)
    pl.semaphore_signal(barrier, 1, device_id=partner, device_id_type=MESH)
    for k in range(1, nx):
        pl.semaphore_signal(barrier, 1, device_id=far_id(k), device_id_type=MESH)
    pl.semaphore_wait(barrier, (n - 1) + 2 + (nx - 1))

    U, V, MIX, GATE, UP, DOWN = 0, 1, 2, 3, 3 + GSUB, 3 + GSUB + USUB
    cuts = df // 128
    bufs = (u_buf, v_buf, mix_buf) + (gate_buf,) * GSUB + (up_buf,) * USUB + (down_buf,) * cuts
    gates, ups = range(GATE, UP), range(UP, DOWN)
    downs = [range(DOWN + p * cuts // parts, DOWN + (p + 1) * cuts // parts) for p in range(parts)]
    streams = len(bufs)
    dc = df // parts
    steps = {
        (1, True): jnp.where(odd == 0, 3, 1),
        (1, False): jnp.where(odd == 0, 1, 2),
        (-1, True): jnp.where(odd == 1, 3, 1),
        (-1, False): jnp.where(odd == 1, 1, 2),
    }

    def view(k, slot, who, h):
        ref = bufs[k]
        if k < GATE:
            count = ref.shape[1] // 2
            return ref.at[slot, pl.ds(pl.multiple_of(who * count, 16), count), :]
        if k < DOWN:
            subs, sub = (GSUB, k - GATE) if k < UP else (USUB, k - UP)
            count = dr // (2 * subs)
            first = (who * subs + sub) * count
            sl = pl.ds(pl.multiple_of(first, 16), count)
            return ref.at[slot, sl, pl.ds(0, widths[h])]
        count = heights[h] // 2
        sl = pl.ds(pl.multiple_of(who * count, 16), count)
        return ref.at[slot, sl, pl.ds((k - DOWN) * 128, 128)]

    def z_copy(k, src, dst, step, h, sem):
        return remote(
            view(k, src, g, h),
            view(k, dst, g, h),
            z_send.at[k, sem],
            z_recv.at[k, dst],
            {"fs": jnp.clip(i + step, 0, n - 1)},
        )

    def y_copy(k, j, who, h):
        ref = view(k, j, who, h)
        return remote(ref, ref, y_send.at[k, j], y_recv.at[k, j], across)

    def stride(k, way, same=True):
        return 1 if k < GATE else steps[way, same]

    def inside(target):
        return jnp.logical_and(target >= 0, target < n)

    def both_halves(f):
        for h in range(2):

            @pl.when(m == h)
            def _():
                f(h)

    def own_each(k, h, act_on, only=None):
        for way in (1, -1):
            for same in (True, False):
                if k < GATE and not same:
                    continue
                step = way * stride(k, way, same)
                fits = inside(i + step)
                if k >= GATE:
                    fits = jnp.logical_and(fits, m == (h if same else 1 - h))
                if only is not None:
                    fits = jnp.logical_and(fits, only)
                src = i if same else n
                sem = n + (0 if way > 0 else 1) + (0 if same else 2)

                @pl.when(fits)
                def _():
                    act_on(z_copy(k, src, i, step, h, sem))

    def own(k, h=0):
        own_each(k, h, lambda copy: copy.start())

    def service(k, s, h=None, side="any"):
        if s >= n:
            return
        if k >= GATE and h is None:
            service(k, s, 0, side)
            service(k, s, 1, side)
            return
        for way in (1, -1):
            j = i - way * s
            here = inside(j)
            if h is not None:
                here = jnp.logical_and(here, m == h)
            if side != "any":
                here = jnp.logical_and(here, odd == (1 if (way > 0) == (side == "in") else 0))
            step = way * stride(k, way)

            @pl.when(here)
            def _():
                z_copy(k, j, j, step, h, j).wait_recv()

                @pl.when(inside(i + step))
                def _():
                    z_copy(k, j, j, step, h, j).start()

                y_copy(k, j, g, h).start()

    def run(k, begin, end, h=None):
        for s in range(begin, end):
            service(k, s, h)

    def finish(k):
        def each(h):
            for s in range(1, n):
                y_copy(k, lax.rem(i + s, n), 1 - g, h).wait_recv()

        if k < GATE:
            each(0)
        else:
            both_halves(each)

    def own_down(p):
        if p < parts:
            for k in downs[p]:
                own(k, 0)
                own(k, 1)

    def finish_all(ks):
        for k in ks:
            finish(k)

    def drain(k):
        for h in range(1 if k < GATE else 2):
            own_each(k, h, lambda copy: copy.wait_send())

        def each(h):
            for s in range(1, n):
                j = lax.rem(i + s, n)
                y_copy(k, j, g, h).wait_send()
                for way in (1, -1):
                    step = way * stride(k, way)

                    @pl.when(jnp.logical_and(way * (i - j) > 0, inside(i + step)))
                    def _():
                        z_copy(k, j, j, step, h, j).wait_send()

        if k < GATE:
            each(0)
        else:
            both_halves(each)

    def chunk(h):
        return pl.ds(h * rt, rt)

    def ag_x(k, h):
        return remote(
            tokens.at[chunk(h), :],
            tok_buf.at[t, chunk(h), :],
            a_send.at[k, h],
            a_recv.at[t, h],
            far_id(k) if k else partner,
        )

    def ag_fwd(k, h):
        slot = far(k) * 2 + c
        ref = tok_buf.at[slot, chunk(h), :]
        return remote(ref, ref, a_fwd.at[k, h], a_recv.at[slot, h], partner)

    def ag_in(k, h):
        slot = far(k) * 2 + 1 - c
        ref = tok_buf.at[slot, chunk(h), :]
        return remote(ref, ref, a_fwd.at[0, h], a_recv.at[slot, h], partner)

    def rchunk(q):
        return pl.ds(q * ct, ct)

    def block(e, slot, q):
        return res_buf.at[e, slot, rchunk(q), :]

    def gx(k, q):
        return remote(block(0, t, q), block(0, t, q), gx_send.at[k, q], g_recv.at[0, t, q], far_id(k))

    def gz(q):
        return remote(block(0, t, q), block(1, t, q), gz_send.at[q], g_recv.at[1, t, q], beside)

    def gd(e, k, q):
        slot = far(k) * 2 + c
        ref = block(e, slot, q)
        return remote(ref, ref, gd_send.at[e, k, q], g_recv.at[e, slot, q], partner)

    def gd_in(e, k, q):
        slot = far(k) * 2 + 1 - c
        ref = block(e, slot, q)
        return remote(ref, ref, gd_send.at[e, k, q], g_recv.at[e, slot, q], partner)

    def gfz(k, q):
        slot = far(k) * 2 + c
        return remote(
            block(0, slot, q), block(1, slot, q), gfz_send.at[k, q], g_recv.at[1, slot, q], beside
        )

    def gfx(k, q):
        return remote(block(1, t, q), block(1, t, q), gfx_send.at[k, q], g_recv.at[1, t, q], far_id(k))

    def g_start(q):
        for k in range(1, nx):
            gx(k, q).start()
        gz(q).start()
        gd(0, 0, q).start()

    def g_first(q):
        for k in range(1, nx):
            gd(0, k, q).wait_recv()
            if q < DIAG:
                gfz(k, q).start()
            gd(0, k, q).start()
        gd(1, 0, q).wait_recv()
        if q >= DIAG:
            for k in range(1, nx):
                gfx(k, q).start()
        gd(1, 0, q).start()

    def g_second(q):
        for k in range(1, nx):
            gd(1, k, q).wait_recv()
            gd(1, k, q).start()

    def g_ready(e, q):
        for k in range(nx):
            gd_in(e, k, q).wait_recv()

    def g_drain():
        for q in range(C):
            gz(q).wait_send()
            for e in range(2):
                for k in range(nx):
                    gd(e, k, q).wait_send()
            for k in range(1, nx):
                gx(k, q).wait_send()
                if q < DIAG:
                    gfz(k, q).wait_send()
                else:
                    gfx(k, q).wait_send()

    bw = dt // parts

    def weight(buf, owner, p):
        ws = [buf[owner * per + q, :, p * dc : (p + 1) * dc] for q in range(per)]
        return ws[0] if per == 1 else jnp.concatenate(ws, axis=1)

    def pair_copy(r, p, xo, e, h):
        return remote(
            give_buf.at[p, xo, e, h],
            pair_buf.at[p, xo, e, h],
            p_send.at[p, xo, e, h],
            p_recv.at[p, xo, e, h],
            partner,
        )

    def partials(r, p, xo, e, h, left, buf):
        right = jnp.concatenate(
            [weight(buf, xo * 2 + 1 - c, p), weight(buf, xo * 2 + c, p)], axis=1
        )
        value = jnp.dot(left, right, preferred_element_type=f32)
        give_buf[p, xo, e, h] = value[:, :bw].astype(bf16)
        pair_copy(r, p, xo, e, h).start()
        keep[p, xo, e, h] = value[:, bw:]

    def both(r, p, xo, e, h):
        pair_copy(r, p, xo, e, h).wait_recv()
        return keep[p, xo, e, h] + pair_buf[p, xo, e, h].astype(f32)

    def mix_copy(p, k, h, slot):
        xo = far(k)
        return remote(
            send_buf.at[p, xo, 0, h],
            far_buf.at[p, slot, 0, h],
            f_send.at[p, xo, 0, h],
            f_recv.at[p, slot, 0, h],
            far_id(k),
        )

    def far_copy(p, src, dst, device):
        return remote(
            send_buf.at[(p,) + src],
            far_buf.at[(p,) + dst],
            f_send.at[(p,) + src],
            f_recv.at[(p,) + dst],
            device,
        )

    def x_one(p, k, e, h):
        return far_copy(p, (far(k), e, h), (x, e, h), far_id(k))

    def x_one_in(p, k, e, h):
        return far_copy(p, (far(k), e, h), (far(k), e, h), far_id(k))

    def z_one(p, k, h):
        return far_copy(p, (far(k), 1, h), (far(k), 0, h), beside)

    def z_two(p, h):
        return far_copy(p, (x, 1, h), (x, 0, h), beside)

    def x_two(p, k, h):
        return far_copy(p, (far(k), 0, h), (x, 1, h), far_id(k))

    def x_two_in(p, k, h):
        return far_copy(p, (far(k), 0, h), (far(k), 1, h), far_id(k))

    def arrived(p, a, e, h):
        return far_buf[p, a, e, h].astype(f32)

    def factor(rows_in):
        total = jnp.zeros((rows_in.shape[0], 1), f32)
        for q in range(n_tp):
            part = rows_in[:, q * dt : (q + 1) * dt].astype(f32)
            total = total + jnp.sum(part * part, axis=1, keepdims=True)
        return lax.rsqrt(total / (n_tp * dt) + eps)

    def column(gain, s):
        lanes = gain[0:1, pl.ds(pl.multiple_of(i * dr + s * 128, 128), 128)]
        return jnp.broadcast_to(lanes, (128, 128)).T[:, :1]

    for h in range(H):
        for k in list(range(1, nx)) + [0]:
            ag_x(k, h).start()
    loads[0].wait()
    loads[1].wait()
    for w, scale, buf in ((0, u_scale, u_buf), (1, v_scale, v_buf)):
        for s in range(dr // 128):
            sl = slice(s * 128, (s + 1) * 128)
            gain = column(mix_gain, s)
            buf[i, sl, :] = (uv_stage[w, sl, :] * gain * scale[0:1, :]).astype(bf16)
        own((U, V)[w])
    loads[2].wait()
    mix_buf[i] = (mix_stage[...] * mix_scale[0:1, :]).astype(bf16)

    def lane_row(scale, lo, hi):
        if scale.shape[0] == 1:
            return scale[0:1, lo:hi]
        return jnp.concatenate([scale[r : r + 1, :] for r in range(lo // 128, hi // 128)], axis=1)

    def cast_in(stage, scale, buf):
        for s in range(dr // 128):
            sl = slice(s * 128, (s + 1) * 128)
            gain = column(ffn_gain, s)
            for h, (lo, hi) in enumerate(((0, wide), (wide, ff))):
                slot = jnp.where(m == h, i, n)
                buf[slot, sl, : hi - lo] = (
                    stage[sl, lo:hi] * gain * lane_row(scale, lo, hi)
                ).astype(bf16)
                if hi - lo < widths[h]:
                    buf[slot, sl, hi - lo : widths[h]] = jnp.zeros(
                        (128, widths[h] - hi + lo), bf16
                    )

    loads[3].wait()
    cast_in(gate_stage, gate_scale, gate_buf)
    loads[4].wait()
    cast_in(up_stage, up_scale, up_buf)
    loads[5].wait()
    for h, (lo, hi) in enumerate(((0, wide), (wide, ff))):
        slot = jnp.where(m == h, i, n)
        down_buf[slot, : hi - lo, :] = (silu_buf[lo:hi, :df] * down_scale[0:1, :]).astype(bf16)

    @pl.when(m == 1)
    def _():
        for j in range(n):
            if padded < wide:
                gate_buf[j, :, padded:] = jnp.zeros((dr, wide - padded), bf16)
                up_buf[j, :, padded:] = jnp.zeros((dr, wide - padded), bf16)
            down_buf[j, rest:, :] = jnp.zeros((wide - rest, df), bf16)

    for s in range(1, n):
        service(U, s)
        service(V, s)
        if s == max(n - 2, 1):
            own(MIX)
    near = max(n - 1, 2)

    def own_at(ks, half, who):
        for k in ks:
            own_each(k, half, lambda copy: copy.start(), m == who)

    def service_all(ks, s, h=None, side="any"):
        for k in ks:
            service(k, s, h, side)

    own_at(gates, 0, 1)
    run(MIX, 1, near, 0)
    own_at(gates, 0, 0)
    for h in range(H):
        for k in range(1, nx):
            ag_fwd(k, h).wait_recv()
            ag_fwd(k, h).start()
    for h in range(H):
        for k in range(nx):
            ag_in(k, h).wait_recv()
    loads[6].wait()
    finish(U)
    service(MIX, 1, 1)
    finish(V)

    groups, span = spatial.shape[0], spatial.shape[1]
    lanes = width // groups
    causal = lax.broadcasted_iota(jnp.int32, (span, span), 0) >= lax.broadcasted_iota(
        jnp.int32, (span, span), 1
    )
    tilt = [jnp.broadcast_to(bias[q : q + 1, :], (span, span)).T[:, :1] for q in range(groups)]

    def gather_rows(pieces):
        return jnp.concatenate(pieces, axis=1)

    for h in range(H):
        left = gather_rows([tok_buf[q, chunk(h), :] for q in range(n_tp)])
        inv = factor(left)
        u = gelu(jnp.dot(left, u_buf[...].reshape(-1, width), preferred_element_type=f32) * inv)
        v = jnp.dot(left, v_buf[...].reshape(-1, width), preferred_element_type=f32) * inv
        v = gelu(v).astype(bf16)
        for q in range(groups):
            mat = jnp.where(causal, spatial[q].astype(f32), 0.0).astype(bf16)
            cols = slice(q * lanes, (q + 1) * lanes)
            for b in range(rt // span):
                sl = slice(b * span, (b + 1) * span)
                mixed = jnp.dot(mat, v[sl, cols], preferred_element_type=f32) + tilt[q]
                gated[h * rt + b * span : h * rt + (b + 1) * span, cols] = (
                    u[sl, cols] * mixed
                ).astype(bf16)
        if h == 0:
            run(MIX, 2, near, 1)
    run(MIX, near, n)
    for k in gates:
        own(k, 1)
    service_all(gates, 1, 0, "in")
    for k in ups:
        own(k, 0)
    finish(MIX)

    for k in range(1, nx):
        for h in range(H):
            for p in range(parts):
                partials(0, p, far(k), 0, h, gated[chunk(h), :], mix_buf)
        for h in range(H):
            for p in range(parts):
                send_buf[p, far(k), 0, h] = both(0, p, far(k), 0, h).astype(bf16)
                mix_copy(p, k, h, x).start()
    for h in range(H):
        for p in range(parts):
            partials(0, p, x, 0, h, gated[chunk(h), :], mix_buf)
    for h in range(H):
        for p in range(parts):
            total = both(0, p, x, 0, h)
            for k in range(1, nx):
                mix_copy(p, k, h, far(k)).wait_recv()
                total = total + arrived(p, far(k), 0, h)
            cols = slice(p * bw, (p + 1) * bw)
            res_buf[0, t, chunk(h), cols] = (
                tok_buf[t, chunk(h), cols].astype(f32) + total
            ).astype(bf16)
        for q in range(h * (C // H), (h + 1) * (C // H)):
            g_start(q)
        if h == 0:
            service(GATE, 1, 1)
            service_all(gates, 1, 0, "out")
    service_all(ups, 1, 0, "in")
    for k in ups:
        own(k, 1)
    own_down(0)
    g_first(0)
    service_all(gates[1:], 1, 1)
    service(GATE, 2)
    g_first(1)
    service_all(gates[1:], 2)
    for k in gates:
        run(k, 3, n)
    g_first(2)
    service_all(ups, 1, 0, "out")
    g_first(3)
    finish_all(gates)

    def gate_tiles(e, begin, end):
        def body(b, carry):
            sl = pl.ds(pl.multiple_of(b * ct, 64), ct)
            left = gather_rows([res_buf[e, q, sl, :] for q in range(n_tp)])
            inv = factor(left)
            a = jnp.dot(left, gate_buf[:n].reshape(-1, wide), preferred_element_type=f32) * inv
            silu_buf[pl.ds(pl.multiple_of(e * rows + b * ct, 64), ct), :] = (
                a / (1.0 + jnp.exp(-a)) * inv
            )
            return carry

        lax.fori_loop(begin, end, body, 0)

    def up_tiles(e):
        def body(b, carry):
            sl = pl.ds(pl.multiple_of(b * ct, 64), ct)
            flat = pl.ds(pl.multiple_of(e * rows + b * ct, 64), ct)
            left = gather_rows([res_buf[e, q, sl, :] for q in range(n_tp)])
            a = jnp.dot(left, up_buf[:n].reshape(-1, wide), preferred_element_type=f32)
            act[flat, :] = (silu_buf[flat, :] * a).astype(bf16)
            return carry

        lax.fori_loop(0, C, body, 0)

    for q in range(C):
        g_ready(0, q)
    gate_tiles(0, 0, C)
    for q in range(C):
        g_second(q)
        for k in ups[q : q + 1]:
            service(k, 1, 1)
            service(k, 2)
            run(k, 3, n)
        if q == 1:
            service_all(downs[0], 1, 0, "in")
            own_down(1)
        if q == C - 2:
            for e in range(C):
                g_ready(1, e) if e < C - 2 else None
            gate_tiles(1, 0, C - 2)
    g_ready(1, C - 2)
    g_ready(1, C - 1)
    gate_tiles(1, C - 2, C)
    for k in downs[0][:1]:
        service(k, 1, 1)
        service(k, 2, 1)
        run(k, 3, n, 1)
    finish_all(ups)
    up_tiles(0)
    service_all(downs[0], 1, 0, "out")
    for k in downs[0][1:]:
        service(k, 1, 1)
        service(k, 2, 1)
        run(k, 3, n, 1)
    up_tiles(1)
    for k in downs[0]:
        service(k, 2, 0)
        run(k, 3, n, 0)

    for p in range(parts):
        for k in range(1, nx + 1):
            for h in range(H):
                pair_copy(0, p, far(k), 0, h).wait_send()
                if k < nx:
                    mix_copy(p, k, h, x).wait_send()

    def z_first(p, h):
        return h == 1

    def sum_first(p):
        order = [(e, k, h) for e in (1, 0) for k in range(1, nx + 1) for h in range(H)]

        def pass_on(e, k, h):
            xo = far(k)
            value = both(1, p, xo, e, h)
            if not z_first(p, h) and k < nx:
                send_buf[p, xo, e, h] = value.astype(bf16)
                x_one(p, k, e, h).start()
            elif z_first(p, h) and e == 1:
                send_buf[p, xo, 1, h] = value.astype(bf16)
                z_one(p, k, h).start()
            else:
                keep[p, xo, e, h] = value

        lag = 4
        for a, (e, k, h) in enumerate(order):
            left = act[e * rows + h * rt : e * rows + (h + 1) * rt, :]
            partials(1, p, far(k), e, h, left, down_buf)
            if a >= lag:
                pass_on(*order[a - lag])
        for a in range(len(order) - lag, len(order)):
            pass_on(*order[a])

    def sum_second(p):
        for h in range(H):
            if z_first(p, h):
                for k in range(1, nx):
                    z_one(p, k, h).wait_recv()
                    send_buf[p, far(k), 0, h] = (
                        keep[p, far(k), 0, h] + arrived(p, far(k), 0, h)
                    ).astype(bf16)
                    x_two(p, k, h).start()
            else:
                value = keep[p, x, 1, h]
                for k in range(1, nx):
                    x_one_in(p, k, 1, h).wait_recv()
                    value = value + arrived(p, far(k), 1, h)
                send_buf[p, x, 1, h] = value.astype(bf16)
                z_two(p, h).start()

    def sum_last(p):
        cols = slice(p * bw, (p + 1) * bw)
        for h in range(H):
            total = keep[p, x, 0, h]
            if z_first(p, h):
                z_one(p, nx, h).wait_recv()
                total = total + arrived(p, x, 0, h)
                for k in range(1, nx):
                    x_two_in(p, k, h).wait_recv()
                    total = total + arrived(p, far(k), 1, h)
            else:
                for k in range(1, nx):
                    x_one_in(p, k, 0, h).wait_recv()
                    total = total + arrived(p, far(k), 0, h)
                z_two(p, h).wait_recv()
                total = total + arrived(p, x, 0, h)
            out[chunk(h), cols] = (
                res_buf[0, t, chunk(h), cols].astype(f32) + total
            ).astype(bf16)

    def sum_drain(p):
        for h in range(H):
            for k in range(1, nx + 1):
                for e in range(2):
                    pair_copy(1, p, far(k), e, h).wait_send()
                if z_first(p, h):
                    z_one(p, k, h).wait_send()
                    if k < nx:
                        x_two(p, k, h).wait_send()
                elif k < nx:
                    for e in range(2):
                        x_one(p, k, e, h).wait_send()
            if not z_first(p, h):
                z_two(p, h).wait_send()

    for p in range(1, parts):
        service_all(downs[p], 1, 0, "in")
    finish_all(downs[0])
    for p in range(1, parts):
        for k in downs[p][:1]:
            service(k, 1, 1)
            service(k, 2, 1)
            run(k, 3, n, 1)
    sum_first(0)
    for p in range(1, parts):
        for k in downs[p][1:]:
            service(k, 1, 1)
            service(k, 2, 1)
            run(k, 3, n, 1)
        service_all(downs[p], 1, 0, "out")
        for k in downs[p]:
            service(k, 2, 0)
            run(k, 3, n, 0)
        finish_all(downs[p])
        sum_first(p)
    for p in range(parts):
        sum_second(p)
    for p in range(parts):
        sum_last(p)

    for p in range(parts):
        sum_drain(p)
    for h in range(H):
        for k in range(nx):
            ag_x(k, h).wait_send()
        for k in range(1, nx):
            ag_fwd(k, h).wait_send()
    g_drain()
    for k in range(streams):
        drain(k)


def lane_rows(scale):
    return scale.reshape(-1, 128) if scale.shape[0] % 128 == 0 else scale.reshape(1, -1)


def local(
    dims,
    tokens,
    mix_gain,
    w_u,
    w_v,
    u_scale,
    v_scale,
    spatial,
    spatial_bias,
    w_mix,
    mix_scale,
    ffn_gain,
    w_gate,
    w_up,
    gate_scale,
    up_scale,
    w_down,
    down_scale,
):
    n, n_tp = dims
    nx = n_tp // 2
    rows, dt = tokens.shape
    dr, ff = w_gate.shape
    df = mix_scale.shape[1]
    parts = 2 if df % 256 == 0 else 1
    streams = 3 + GSUB + USUB + df // 128
    wide = up_to(-(-ff // 2), 128)
    rt, bw = rows // H, dt // parts
    hbm = pl.BlockSpec(memory_space=pl.ANY)
    vmem = pl.BlockSpec(memory_space=pltpu.VMEM)
    dma = pltpu.SemaphoreType.DMA
    sums = (parts, nx, 2, H, rt, bw)
    return pl.pallas_call(
        functools.partial(layer_kernel, (n, n_tp, parts)),
        out_shape=jax.ShapeDtypeStruct((rows, dt), bf16),
        in_specs=[hbm, vmem, vmem] + [hbm] * 6 + [vmem] * 8,
        out_specs=vmem,
        scratch_shapes=[
            pltpu.VMEM((2,) + w_u.shape, f32),
            pltpu.VMEM(w_mix.shape, f32),
            pltpu.VMEM(w_gate.shape, f32),
            pltpu.VMEM(w_up.shape, f32),
            pltpu.VMEM((n,) + w_u.shape, bf16),
            pltpu.VMEM((n,) + w_v.shape, bf16),
            pltpu.VMEM((n,) + w_mix.shape, bf16),
            pltpu.VMEM((n + 1, dr, wide), bf16),
            pltpu.VMEM((n + 1, dr, wide), bf16),
            pltpu.VMEM((n + 1, wide, df), bf16),
            pltpu.VMEM((n_tp, rows, dt), bf16),
            pltpu.VMEM((2, n_tp, rows, dt), bf16),
            pltpu.VMEM((rows, w_u.shape[1]), bf16),
            pltpu.VMEM((2 * rows, wide), f32),
            pltpu.VMEM((2 * rows, wide), bf16),
            pltpu.VMEM(sums, bf16),
            pltpu.VMEM(sums, bf16),
            pltpu.VMEM(sums, f32),
            pltpu.VMEM(sums, bf16),
            pltpu.VMEM(sums, bf16),
            dma((7,)),
            dma((streams, n + 4)),
            dma((streams, n)),
            dma((streams, n)),
            dma((streams, n)),
            dma((nx, H)),
            dma((nx, H)),
            dma((n_tp, H)),
            dma((nx, C)),
            dma((C,)),
            dma((2, nx, C)),
            dma((nx, C)),
            dma((nx, C)),
            dma((2, n_tp, C)),
            dma((parts, nx, 2, H)),
            dma((parts, nx, 2, H)),
            dma((parts, nx, 2, H)),
            dma((parts, nx, 2, H)),
        ],
        compiler_params=pltpu.CompilerParams(
            collective_id=0, has_side_effects=True, vmem_limit_bytes=67000000
        ),
    )(
        tokens,
        mix_gain.reshape(1, -1),
        ffn_gain.reshape(1, -1),
        w_u,
        w_v,
        w_mix,
        w_gate,
        w_up,
        w_down,
        u_scale.reshape(1, -1),
        v_scale.reshape(1, -1),
        spatial,
        spatial_bias,
        mix_scale,
        lane_rows(gate_scale),
        lane_rows(up_scale),
        down_scale,
    )


def solution(mesh):
    placed = (
        P(("grp", "fs"), "tp"),
        P(),
        P("fs", "tp"),
        P("fs", "tp"),
        P("tp"),
        P("tp"),
        P("tp", None, None),
        P("tp", None),
        P("tp", "fs"),
        P(None, "fs"),
        P(),
        P("fs", "tp"),
        P("fs", "tp"),
        P("tp"),
        P("tp"),
        P("tp", "fs"),
        P(None, "fs"),
    )
    dims = (mesh.shape["fs"], mesh.shape["tp"])
    return jax.shard_map(
        functools.partial(local, dims),
        mesh=mesh,
        in_specs=placed,
        out_specs=P(("grp", "fs"), "tp"),
        check_vma=False,
    )
```

```python
import functools

import jax
import jax.numpy as jnp
from jax import lax
from jax.experimental import pallas as pl
from jax.experimental.pallas import tpu as pltpu
from jax.sharding import PartitionSpec as P

MESH = pl.DeviceIdType.MESH
eps = 1e-06
H = 2
C = 4
DIAG = 0
GSUB = 2
USUB = 4
half_root = 0.7071067811865476
f32 = jnp.float32
bf16 = jnp.bfloat16


def gelu(a):
    return 0.5 * a * (1.0 + lax.erf(a * half_root))


def up_to(a, b):
    return -(-a // b) * b


def layer_kernel(
    dims,
    tokens,
    mix_gain,
    ffn_gain,
    w_u,
    w_v,
    w_mix,
    w_gate,
    w_up,
    w_down,
    u_scale,
    v_scale,
    spatial,
    bias,
    mix_scale,
    gate_scale,
    up_scale,
    down_scale,
    out,
    uv_stage,
    mix_stage,
    gate_stage,
    up_stage,
    u_buf,
    v_buf,
    mix_buf,
    gate_buf,
    up_buf,
    down_buf,
    tok_buf,
    res_buf,
    gated,
    silu_buf,
    act,
    give_buf,
    pair_buf,
    keep,
    send_buf,
    far_buf,
    load_sem,
    z_send,
    z_recv,
    y_send,
    y_recv,
    a_send,
    a_fwd,
    a_recv,
    gx_send,
    gz_send,
    gd_send,
    gfz_send,
    gfx_send,
    g_recv,
    p_send,
    p_recv,
    f_send,
    f_recv,
):
    n, n_tp, parts = dims
    nx = n_tp // 2
    i = lax.axis_index("fs")
    g = lax.axis_index("grp")
    t = lax.axis_index("tp")
    x, c = t // 2, t % 2
    quad = i % 4
    odd = i % 2
    m = jnp.where(jnp.logical_or(quad == 0, quad == 3), 1, 0)
    rows, dt = tokens.shape
    dr, ff = w_gate.shape
    df = w_down.shape[1]
    per = dt // df
    rt = rows // H
    ct = rows // C
    wide = gate_buf.shape[2]
    rest = ff - wide
    padded = up_to(rest, 128)
    widths = (wide, padded)
    heights = (wide, rest)
    partner = {"tp": x * 2 + 1 - c}
    across = {"grp": 1 - g}
    beside = {"fs": i + 1 - 2 * odd}

    def far(k):
        return lax.rem(x + k, nx)

    def far_id(k):
        return {"tp": far(k) * 2 + c}

    def remote(src, dst, ss, rs, device):
        return pltpu.make_async_remote_copy(
            src_ref=src,
            dst_ref=dst,
            send_sem=ss,
            recv_sem=rs,
            device_id=device,
            device_id_type=MESH,
        )

    width = w_u.shape[1]
    loads = [
        pltpu.make_async_copy(w_u, uv_stage.at[0], load_sem.at[0]),
        pltpu.make_async_copy(w_v, uv_stage.at[1], load_sem.at[1]),
        pltpu.make_async_copy(w_mix, mix_stage, load_sem.at[2]),
        pltpu.make_async_copy(w_gate, gate_stage, load_sem.at[3]),
        pltpu.make_async_copy(w_up, up_stage, load_sem.at[4]),
        pltpu.make_async_copy(w_down, silu_buf.at[pl.ds(0, ff), pl.ds(0, df)], load_sem.at[5]),
        pltpu.make_async_copy(tokens, tok_buf.at[t], load_sem.at[6]),
    ]
    for copy in loads:
        copy.start()

    barrier = pltpu.get_barrier_semaphore()
    for k in range(1, n):
        pl.semaphore_signal(barrier, 1, device_id={"fs": (i + k) % n}, device_id_type=MESH)
    pl.semaphore_signal(barrier, 1, device_id=across, device_id_type=MESH)
    pl.semaphore_signal(barrier, 1, device_id=partner, device_id_type=MESH)
    for k in range(1, nx):
        pl.semaphore_signal(barrier, 1, device_id=far_id(k), device_id_type=MESH)
    pl.semaphore_wait(barrier, (n - 1) + 2 + (nx - 1))

    U, V, MIX = 0, 1, 2
    GATE = MIX + parts
    UP = GATE + GSUB
    DOWN = UP + USUB
    cuts = df // 128
    bufs = (u_buf, v_buf) + (mix_buf,) * parts + (gate_buf,) * GSUB + (up_buf,) * USUB + (down_buf,) * cuts
    gates, ups = range(GATE, UP), range(UP, DOWN)
    downs = [range(DOWN + p * cuts // parts, DOWN + (p + 1) * cuts // parts) for p in range(parts)]
    streams = len(bufs)
    dc = df // parts
    steps = {
        (1, True): jnp.where(odd == 0, 3, 1),
        (1, False): jnp.where(odd == 0, 1, 2),
        (-1, True): jnp.where(odd == 1, 3, 1),
        (-1, False): jnp.where(odd == 1, 1, 2),
    }

    def view(k, slot, who, h):
        ref = bufs[k]
        if k < GATE:
            count = ref.shape[1] // 2
            first, cols = (0, width) if k < MIX else ((k - MIX) * dc, dc)
            sl = pl.ds(pl.multiple_of(who * count, 16), count)
            return ref.at[slot, sl, pl.ds(first, cols)]
        if k < DOWN:
            subs, sub = (GSUB, k - GATE) if k < UP else (USUB, k - UP)
            count = dr // (2 * subs)
            first = (who * subs + sub) * count
            sl = pl.ds(pl.multiple_of(first, 16), count)
            return ref.at[slot, sl, pl.ds(0, widths[h])]
        count = heights[h] // 2
        sl = pl.ds(pl.multiple_of(who * count, 16), count)
        return ref.at[slot, sl, pl.ds((k - DOWN) * 128, 128)]

    def z_copy(k, src, dst, step, h, sem):
        return remote(
            view(k, src, g, h),
            view(k, dst, g, h),
            z_send.at[k, sem],
            z_recv.at[k, dst],
            {"fs": jnp.clip(i + step, 0, n - 1)},
        )

    def y_copy(k, j, who, h):
        ref = view(k, j, who, h)
        return remote(ref, ref, y_send.at[k, j], y_recv.at[k, j], across)

    def stride(k, way, same=True):
        return 1 if k < GATE else steps[way, same]

    def inside(target):
        return jnp.logical_and(target >= 0, target < n)

    def both_halves(f):
        for h in range(2):

            @pl.when(m == h)
            def _():
                f(h)

    def own_each(k, h, act_on, only=None, side=None):
        for way in (1, -1):
            for same in (True, False):
                if k < GATE and not same:
                    continue
                step = way * stride(k, way, same)
                fits = inside(i + step)
                if k >= GATE:
                    fits = jnp.logical_and(fits, m == (h if same else 1 - h))
                if only is not None:
                    fits = jnp.logical_and(fits, only)
                if side is not None:
                    to_pair = jnp.logical_and(odd == (0 if way > 0 else 1), not same)
                    fits = jnp.logical_and(fits, to_pair == (side == "in"))
                src = i if same else n
                sem = {(1, True): i, (-1, True): n, (1, False): n + 1, (-1, False): n + 2}[way, same]

                @pl.when(fits)
                def _():
                    act_on(z_copy(k, src, i, step, h, sem))

    def own(k, h=0, side=None):
        own_each(k, h, lambda copy: copy.start(), None, side)

    def service(k, s, h=None, side="any"):
        if s >= n:
            return
        if k >= GATE and h is None:
            service(k, s, 0, side)
            service(k, s, 1, side)
            return
        for way in (1, -1):
            j = i - way * s
            here = inside(j)
            if h is not None:
                here = jnp.logical_and(here, m == h)
            if side != "any":
                here = jnp.logical_and(here, odd == (1 if (way > 0) == (side == "in") else 0))
            step = way * stride(k, way)

            @pl.when(here)
            def _():
                z_copy(k, j, j, step, h, j).wait_recv()

                @pl.when(inside(i + step))
                def _():
                    z_copy(k, j, j, step, h, j).start()

                y_copy(k, j, g, h).start()

    def run(k, begin, end, h=None):
        for s in range(begin, end):
            service(k, s, h)

    def finish(k):
        def each(h):
            for s in range(1, n):
                y_copy(k, lax.rem(i + s, n), 1 - g, h).wait_recv()

        if k < GATE:
            each(0)
        else:
            both_halves(each)

    def own_down(p, side=None):
        if p < parts:
            for k in downs[p]:
                own(k, 0)
                own(k, 1, side)

    def finish_all(ks):
        for k in ks:
            finish(k)

    def drain(k):
        for h in range(1 if k < GATE else 2):
            own_each(k, h, lambda copy: copy.wait_send())

        def each(h):
            for s in range(1, n):
                j = lax.rem(i + s, n)
                y_copy(k, j, g, h).wait_send()
                for way in (1, -1):
                    step = way * stride(k, way)

                    @pl.when(jnp.logical_and(way * (i - j) > 0, inside(i + step)))
                    def _():
                        z_copy(k, j, j, step, h, j).wait_send()

        if k < GATE:
            each(0)
        else:
            both_halves(each)

    def chunk(h):
        return pl.ds(h * rt, rt)

    def ag_x(k, h):
        return remote(
            tokens.at[chunk(h), :],
            tok_buf.at[t, chunk(h), :],
            a_send.at[k, h],
            a_recv.at[t, h],
            far_id(k) if k else partner,
        )

    def ag_fwd(k, h):
        slot = far(k) * 2 + c
        ref = tok_buf.at[slot, chunk(h), :]
        return remote(ref, ref, a_fwd.at[k, h], a_recv.at[slot, h], partner)

    def ag_in(k, h):
        slot = far(k) * 2 + 1 - c
        ref = tok_buf.at[slot, chunk(h), :]
        return remote(ref, ref, a_fwd.at[0, h], a_recv.at[slot, h], partner)

    def rchunk(q):
        return pl.ds(q * ct, ct)

    def block(e, slot, q):
        return res_buf.at[e, slot, rchunk(q), :]

    def gx(k, q):
        return remote(block(0, t, q), block(0, t, q), gx_send.at[k, q], g_recv.at[0, t, q], far_id(k))

    def gz(q):
        return remote(block(0, t, q), block(1, t, q), gz_send.at[q], g_recv.at[1, t, q], beside)

    def gd(e, k, q):
        slot = far(k) * 2 + c
        ref = block(e, slot, q)
        return remote(ref, ref, gd_send.at[e, k, q], g_recv.at[e, slot, q], partner)

    def gd_in(e, k, q):
        slot = far(k) * 2 + 1 - c
        ref = block(e, slot, q)
        return remote(ref, ref, gd_send.at[e, k, q], g_recv.at[e, slot, q], partner)

    def gfz(k, q):
        slot = far(k) * 2 + c
        return remote(
            block(0, slot, q), block(1, slot, q), gfz_send.at[k, q], g_recv.at[1, slot, q], beside
        )

    def gfx(k, q):
        return remote(block(1, t, q), block(1, t, q), gfx_send.at[k, q], g_recv.at[1, t, q], far_id(k))

    def g_start(q):
        for k in range(1, nx):
            gx(k, q).start()
        gz(q).start()
        gd(0, 0, q).start()

    def g_first(q):
        for k in range(1, nx):
            gd(0, k, q).wait_recv()
            if q < DIAG:
                gfz(k, q).start()
            gd(0, k, q).start()
        gd(1, 0, q).wait_recv()
        if q >= DIAG:
            for k in range(1, nx):
                gfx(k, q).start()
        gd(1, 0, q).start()

    def g_second(q):
        for k in range(1, nx):
            gd(1, k, q).wait_recv()
            gd(1, k, q).start()

    def g_ready(e, q):
        for k in range(nx):
            gd_in(e, k, q).wait_recv()

    def g_drain():
        for q in range(C):
            gz(q).wait_send()
            for e in range(2):
                for k in range(nx):
                    gd(e, k, q).wait_send()
            for k in range(1, nx):
                gx(k, q).wait_send()
                if q < DIAG:
                    gfz(k, q).wait_send()
                else:
                    gfx(k, q).wait_send()

    bw = dt // parts

    def weight(buf, owner, p):
        ws = [buf[owner * per + q, :, p * dc : (p + 1) * dc] for q in range(per)]
        return ws[0] if per == 1 else jnp.concatenate(ws, axis=1)

    def pair_copy(r, p, xo, e, h):
        return remote(
            give_buf.at[p, xo, e, h],
            pair_buf.at[p, xo, e, h],
            p_send.at[p, xo, e, h],
            p_recv.at[p, xo, e, h],
            partner,
        )

    def partials(r, p, xo, e, h, left, buf):
        right = jnp.concatenate(
            [weight(buf, xo * 2 + 1 - c, p), weight(buf, xo * 2 + c, p)], axis=1
        )
        value = jnp.dot(left, right, preferred_element_type=f32)
        give_buf[p, xo, e, h] = value[:, :bw].astype(bf16)
        pair_copy(r, p, xo, e, h).start()
        keep[p, xo, e, h] = value[:, bw:]

    def both(r, p, xo, e, h):
        pair_copy(r, p, xo, e, h).wait_recv()
        return keep[p, xo, e, h] + pair_buf[p, xo, e, h].astype(f32)

    def mix_copy(p, k, h, slot):
        xo = far(k)
        return remote(
            send_buf.at[p, xo, 0, h],
            far_buf.at[p, slot, 0, h],
            f_send.at[p, xo, 0, h],
            f_recv.at[p, slot, 0, h],
            far_id(k),
        )

    def far_copy(p, src, dst, device):
        return remote(
            send_buf.at[(p,) + src],
            far_buf.at[(p,) + dst],
            f_send.at[(p,) + src],
            f_recv.at[(p,) + dst],
            device,
        )

    def x_one(p, k, e, h):
        return far_copy(p, (far(k), e, h), (x, e, h), far_id(k))

    def x_one_in(p, k, e, h):
        return far_copy(p, (far(k), e, h), (far(k), e, h), far_id(k))

    def z_one(p, k, h):
        return far_copy(p, (far(k), 1, h), (far(k), 0, h), beside)

    def z_two(p, h):
        return far_copy(p, (x, 1, h), (x, 0, h), beside)

    def x_two(p, k, h):
        return far_copy(p, (far(k), 0, h), (x, 1, h), far_id(k))

    def x_two_in(p, k, h):
        return far_copy(p, (far(k), 0, h), (far(k), 1, h), far_id(k))

    def arrived(p, a, e, h):
        return far_buf[p, a, e, h].astype(f32)

    def factor(rows_in):
        total = jnp.zeros((rows_in.shape[0], 1), f32)
        for q in range(n_tp):
            part = rows_in[:, q * dt : (q + 1) * dt].astype(f32)
            total = total + jnp.sum(part * part, axis=1, keepdims=True)
        return lax.rsqrt(total / (n_tp * dt) + eps)

    def column(gain, s):
        lanes = gain[0:1, pl.ds(pl.multiple_of(i * dr + s * 128, 128), 128)]
        return jnp.broadcast_to(lanes, (128, 128)).T[:, :1]

    for h in range(H):
        for k in list(range(1, nx)) + [0]:
            ag_x(k, h).start()
    loads[0].wait()
    loads[1].wait()
    for w, scale, buf in ((0, u_scale, u_buf), (1, v_scale, v_buf)):
        for s in range(dr // 128):
            sl = slice(s * 128, (s + 1) * 128)
            gain = column(mix_gain, s)
            buf[i, sl, :] = (uv_stage[w, sl, :] * gain * scale[0:1, :]).astype(bf16)
        own((U, V)[w])
    loads[2].wait()
    mix_buf[i] = (mix_stage[...] * mix_scale[0:1, :]).astype(bf16)

    def lane_row(scale, lo, hi):
        if scale.shape[0] == 1:
            return scale[0:1, lo:hi]
        return jnp.concatenate([scale[r : r + 1, :] for r in range(lo // 128, hi // 128)], axis=1)

    def cast_in(stage, scale, buf):
        for s in range(dr // 128):
            sl = slice(s * 128, (s + 1) * 128)
            gain = column(ffn_gain, s)
            for h, (lo, hi) in enumerate(((0, wide), (wide, ff))):
                slot = jnp.where(m == h, i, n)
                buf[slot, sl, : hi - lo] = (
                    stage[sl, lo:hi] * gain * lane_row(scale, lo, hi)
                ).astype(bf16)
                if hi - lo < widths[h]:
                    buf[slot, sl, hi - lo : widths[h]] = jnp.zeros(
                        (128, widths[h] - hi + lo), bf16
                    )

    loads[3].wait()
    cast_in(gate_stage, gate_scale, gate_buf)
    loads[4].wait()
    cast_in(up_stage, up_scale, up_buf)
    loads[5].wait()
    for h, (lo, hi) in enumerate(((0, wide), (wide, ff))):
        slot = jnp.where(m == h, i, n)
        down_buf[slot, : hi - lo, :] = (silu_buf[lo:hi, :df] * down_scale[0:1, :]).astype(bf16)

    @pl.when(m == 1)
    def _():
        for j in range(n):
            if padded < wide:
                gate_buf[j, :, padded:] = jnp.zeros((dr, wide - padded), bf16)
                up_buf[j, :, padded:] = jnp.zeros((dr, wide - padded), bf16)
            down_buf[j, rest:, :] = jnp.zeros((wide - rest, df), bf16)

    for s in range(1, n):
        service(U, s)
        service(V, s)
        if s == max(n - 2, 1):
            for k in range(MIX, GATE):
                own(k)
    near = max(n - 1, 2)
    mixes = range(MIX, GATE)

    def own_at(ks, half, who):
        for k in ks:
            own_each(k, half, lambda copy: copy.start(), m == who)

    def service_all(ks, s, h=None, side="any"):
        for k in ks:
            service(k, s, h, side)

    def far_in(ks):
        if n <= 4:
            for k in ks:
                run(k, 2, n, 1)

    def near_in(ks):
        for k in ks:
            run(k, 1, 2 if n <= 4 else n, 1)

    own_at(gates, 0, 1)
    for s in range(1, near):
        service_all(mixes, s, 0)
    own_at(gates, 0, 0)
    for h in range(H):
        for k in range(1, nx):
            ag_fwd(k, h).wait_recv()
            ag_fwd(k, h).start()
    for h in range(H):
        for k in range(nx):
            ag_in(k, h).wait_recv()
    loads[6].wait()
    finish(U)
    service_all(mixes, 1, 1)
    finish(V)

    groups, span = spatial.shape[0], spatial.shape[1]
    lanes = width // groups
    causal = lax.broadcasted_iota(jnp.int32, (span, span), 0) >= lax.broadcasted_iota(
        jnp.int32, (span, span), 1
    )
    tilt = [jnp.broadcast_to(bias[q : q + 1, :], (span, span)).T[:, :1] for q in range(groups)]

    def gather_rows(pieces):
        return jnp.concatenate(pieces, axis=1)

    for h in range(H):
        left = gather_rows([tok_buf[q, chunk(h), :] for q in range(n_tp)])
        inv = factor(left)
        u = gelu(jnp.dot(left, u_buf[...].reshape(-1, width), preferred_element_type=f32) * inv)
        v = jnp.dot(left, v_buf[...].reshape(-1, width), preferred_element_type=f32) * inv
        v = gelu(v).astype(bf16)
        for q in range(groups):
            mat = jnp.where(causal, spatial[q].astype(f32), 0.0).astype(bf16)
            cols = slice(q * lanes, (q + 1) * lanes)
            for b in range(rt // span):
                sl = slice(b * span, (b + 1) * span)
                mixed = jnp.dot(mat, v[sl, cols], preferred_element_type=f32) + tilt[q]
                gated[h * rt + b * span : h * rt + (b + 1) * span, cols] = (
                    u[sl, cols] * mixed
                ).astype(bf16)
        if h == 0:
            for s in range(2, near):
                service_all(mixes, s, 1)
    for s in range(near, n):
        service_all(mixes, s)
    for k in gates:
        own(k, 1)
    service_all(gates, 1, 0, "in")
    for k in ups:
        own(k, 0)
    for p in range(parts):
        finish(MIX + p)
        for k in range(1, nx):
            for h in range(H):
                partials(0, p, far(k), 0, h, gated[chunk(h), :], mix_buf)
        for h in range(H):
            partials(0, p, x, 0, h, gated[chunk(h), :], mix_buf)
        for k in range(1, nx):
            for h in range(H):
                send_buf[p, far(k), 0, h] = both(0, p, far(k), 0, h).astype(bf16)
                mix_copy(p, k, h, x).start()
    for h in range(H):
        for p in range(parts):
            total = both(0, p, x, 0, h)
            for k in range(1, nx):
                mix_copy(p, k, h, far(k)).wait_recv()
                total = total + arrived(p, far(k), 0, h)
            cols = slice(p * bw, (p + 1) * bw)
            res_buf[0, t, chunk(h), cols] = (
                tok_buf[t, chunk(h), cols].astype(f32) + total
            ).astype(bf16)
        for q in range(h * (C // H), (h + 1) * (C // H)):
            g_start(q)
        if h == 0:
            service_all(gates, 1, 0, "out")
            far_in(gates)
    service_all(ups, 1, 0, "in")
    for k in ups:
        own(k, 1, "in")
    own(DOWN, 0)
    near_in(gates)
    service(GATE, 2, 0)
    service_all(gates[1:], 2, 0)
    for k in gates:
        run(k, 3, n, 0)
    for q in range(C - 1):
        g_first(q)
    service_all(ups, 1, 0, "out")
    g_first(C - 1)
    for k in ups:
        own(k, 1, "out")
    for k in downs[0][1:]:
        own(k, 0)
    if n <= 4:
        service(UP, 1, 1)
    finish_all(gates)

    def gate_tiles(e, begin, end):
        def body(b, carry):
            sl = pl.ds(pl.multiple_of(b * ct, 64), ct)
            left = gather_rows([res_buf[e, q, sl, :] for q in range(n_tp)])
            inv = factor(left)
            a = jnp.dot(left, gate_buf[:n].reshape(-1, wide), preferred_element_type=f32) * inv
            silu_buf[pl.ds(pl.multiple_of(e * rows + b * ct, 64), ct), :] = (
                a / (1.0 + jnp.exp(-a)) * inv
            )
            return carry

        lax.fori_loop(begin, end, body, 0)

    def up_tiles(e, begin, end):
        def body(b, carry):
            sl = pl.ds(pl.multiple_of(b * ct, 64), ct)
            flat = pl.ds(pl.multiple_of(e * rows + b * ct, 64), ct)
            left = gather_rows([res_buf[e, q, sl, :] for q in range(n_tp)])
            a = jnp.dot(left, up_buf[:n].reshape(-1, wide), preferred_element_type=f32)
            act[flat, :] = (silu_buf[flat, :] * a).astype(bf16)
            return carry

        lax.fori_loop(begin, end, body, 0)

    for q in range(C):
        g_ready(0, q)
    gate_tiles(0, 0, C // 2)
    run(UP, 2, n, 0)
    far_in(ups[:1])
    gate_tiles(0, C // 2, C)
    for q in range(C):
        g_second(q)
        for k in ups[max(q, 1) : q + 1]:
            run(k, 2, n, 0)
            far_in([k])
        if q == 1:
            service_all(downs[0], 1, 0, "in")
            for k in downs[0]:
                own(k, 1)
            own_down(1)
        if q == C - 2:
            for e in range(C):
                g_ready(1, e) if e < C - 2 else None
            gate_tiles(1, 0, C - 2)
    near_in(ups[1:] if n <= 4 else ups)
    g_ready(1, C - 2)
    g_ready(1, C - 1)
    gate_tiles(1, C - 2, C)
    far_in(downs[0][:1])
    near_in(downs[0][:1])
    finish_all(ups)
    up_tiles(0, 0, C // 2)
    far_in(downs[0][1:])
    near_in(downs[0][1:])
    up_tiles(0, C // 2, C)
    service_all(downs[0], 1, 0, "out")
    up_tiles(1, 0, C // 2)
    for k in downs[0]:
        run(k, 2, n, 0)
    up_tiles(1, C // 2, C)

    for p in range(parts):
        for k in range(1, nx + 1):
            for h in range(H):
                pair_copy(0, p, far(k), 0, h).wait_send()
                if k < nx:
                    mix_copy(p, k, h, x).wait_send()

    def z_first(p, h):
        return h == 1

    def sum_first(p, hook):
        order = [(e, k, h) for e in (1, 0) for k in range(1, nx + 1) for h in range(H)]

        def pass_on(e, k, h):
            xo = far(k)
            value = both(1, p, xo, e, h)
            if not z_first(p, h) and k < nx:
                send_buf[p, xo, e, h] = value.astype(bf16)
                x_one(p, k, e, h).start()
            elif z_first(p, h) and e == 1:
                send_buf[p, xo, 1, h] = value.astype(bf16)
                z_one(p, k, h).start()
            else:
                keep[p, xo, e, h] = value

        lag = 4
        for a, (e, k, h) in enumerate(order):
            left = act[e * rows + h * rt : e * rows + (h + 1) * rt, :]
            partials(1, p, far(k), e, h, left, down_buf)
            if a >= lag:
                pass_on(*order[a - lag])
            if a == lag:
                hook()
        for a in range(len(order) - lag, len(order)):
            pass_on(*order[a])

    def sum_second(p):
        for h in range(H):
            if z_first(p, h):
                for k in range(1, nx):
                    z_one(p, k, h).wait_recv()
                    send_buf[p, far(k), 0, h] = (
                        keep[p, far(k), 0, h] + arrived(p, far(k), 0, h)
                    ).astype(bf16)
                    x_two(p, k, h).start()
            else:
                value = keep[p, x, 1, h]
                for k in range(1, nx):
                    x_one_in(p, k, 1, h).wait_recv()
                    value = value + arrived(p, far(k), 1, h)
                send_buf[p, x, 1, h] = value.astype(bf16)
                z_two(p, h).start()

    def sum_last(p):
        cols = slice(p * bw, (p + 1) * bw)
        for h in range(H):
            total = keep[p, x, 0, h]
            if z_first(p, h):
                z_one(p, nx, h).wait_recv()
                total = total + arrived(p, x, 0, h)
                for k in range(1, nx):
                    x_two_in(p, k, h).wait_recv()
                    total = total + arrived(p, far(k), 1, h)
            else:
                for k in range(1, nx):
                    x_one_in(p, k, 0, h).wait_recv()
                    total = total + arrived(p, far(k), 0, h)
                z_two(p, h).wait_recv()
                total = total + arrived(p, x, 0, h)
            out[chunk(h), cols] = (
                res_buf[0, t, chunk(h), cols].astype(f32) + total
            ).astype(bf16)

    def sum_drain(p):
        for h in range(H):
            for k in range(1, nx + 1):
                for e in range(2):
                    pair_copy(1, p, far(k), e, h).wait_send()
                if z_first(p, h):
                    z_one(p, k, h).wait_send()
                    if k < nx:
                        x_two(p, k, h).wait_send()
                elif k < nx:
                    for e in range(2):
                        x_one(p, k, e, h).wait_send()
            if not z_first(p, h):
                z_two(p, h).wait_send()

    for p in range(1, parts):
        service_all(downs[p], 1, 0, "in")
    finish_all(downs[0])

    def later(k):
        far_in([k])
        near_in([k])
        service(k, 1, 0, "out")
        run(k, 2, n, 0)

    rest_downs = [k for p in range(1, parts) for k in downs[p]]
    for k in rest_downs[:1]:
        later(k)
    sum_first(0, lambda: [later(k) for k in rest_downs[1:]])
    for p in range(1, parts):
        finish_all(downs[p])
        sum_second(p - 1)
        sum_first(p, lambda: None)
        sum_last(p - 1)
    sum_second(parts - 1)
    sum_last(parts - 1)

    for p in range(parts):
        sum_drain(p)
    for h in range(H):
        for k in range(nx):
            ag_x(k, h).wait_send()
        for k in range(1, nx):
            ag_fwd(k, h).wait_send()
    g_drain()
    for k in range(streams):
        drain(k)


def lane_rows(scale):
    return scale.reshape(-1, 128) if scale.shape[0] % 128 == 0 else scale.reshape(1, -1)


def local(
    dims,
    tokens,
    mix_gain,
    w_u,
    w_v,
    u_scale,
    v_scale,
    spatial,
    spatial_bias,
    w_mix,
    mix_scale,
    ffn_gain,
    w_gate,
    w_up,
    gate_scale,
    up_scale,
    w_down,
    down_scale,
):
    n, n_tp = dims
    nx = n_tp // 2
    rows, dt = tokens.shape
    dr, ff = w_gate.shape
    df = mix_scale.shape[1]
    parts = 2 if df % 256 == 0 else 1
    streams = 2 + parts + GSUB + USUB + df // 128
    wide = up_to(-(-ff // 2), 128)
    rt, bw = rows // H, dt // parts
    hbm = pl.BlockSpec(memory_space=pl.ANY)
    vmem = pl.BlockSpec(memory_space=pltpu.VMEM)
    dma = pltpu.SemaphoreType.DMA
    sums = (parts, nx, 2, H, rt, bw)
    return pl.pallas_call(
        functools.partial(layer_kernel, (n, n_tp, parts)),
        out_shape=jax.ShapeDtypeStruct((rows, dt), bf16),
        in_specs=[hbm, vmem, vmem] + [hbm] * 6 + [vmem] * 8,
        out_specs=vmem,
        scratch_shapes=[
            pltpu.VMEM((2,) + w_u.shape, f32),
            pltpu.VMEM(w_mix.shape, f32),
            pltpu.VMEM(w_gate.shape, f32),
            pltpu.VMEM(w_up.shape, f32),
            pltpu.VMEM((n,) + w_u.shape, bf16),
            pltpu.VMEM((n,) + w_v.shape, bf16),
            pltpu.VMEM((n,) + w_mix.shape, bf16),
            pltpu.VMEM((n + 1, dr, wide), bf16),
            pltpu.VMEM((n + 1, dr, wide), bf16),
            pltpu.VMEM((n + 1, wide, df), bf16),
            pltpu.VMEM((n_tp, rows, dt), bf16),
            pltpu.VMEM((2, n_tp, rows, dt), bf16),
            pltpu.VMEM((rows, w_u.shape[1]), bf16),
            pltpu.VMEM((2 * rows, wide), f32),
            pltpu.VMEM((2 * rows, wide), bf16),
            pltpu.VMEM(sums, bf16),
            pltpu.VMEM(sums, bf16),
            pltpu.VMEM(sums, f32),
            pltpu.VMEM(sums, bf16),
            pltpu.VMEM(sums, bf16),
            dma((7,)),
            dma((streams, n + 3)),
            dma((streams, n)),
            dma((streams, n)),
            dma((streams, n)),
            dma((nx, H)),
            dma((nx, H)),
            dma((n_tp, H)),
            dma((nx, C)),
            dma((C,)),
            dma((2, nx, C)),
            dma((nx, max(DIAG, 1))),
            dma((nx, C)),
            dma((2, n_tp, C)),
            dma((parts, nx, 2, H)),
            dma((parts, nx, 2, H)),
            dma((parts, nx, 2, H)),
            dma((parts, nx, 2, H)),
        ],
        compiler_params=pltpu.CompilerParams(
            collective_id=0, has_side_effects=True, vmem_limit_bytes=67000000
        ),
    )(
        tokens,
        mix_gain.reshape(1, -1),
        ffn_gain.reshape(1, -1),
        w_u,
        w_v,
        w_mix,
        w_gate,
        w_up,
        w_down,
        u_scale.reshape(1, -1),
        v_scale.reshape(1, -1),
        spatial,
        spatial_bias,
        mix_scale,
        lane_rows(gate_scale),
        lane_rows(up_scale),
        down_scale,
    )


def solution(mesh):
    placed = (
        P(("grp", "fs"), "tp"),
        P(),
        P("fs", "tp"),
        P("fs", "tp"),
        P("tp"),
        P("tp"),
        P("tp", None, None),
        P("tp", None),
        P("tp", "fs"),
        P(None, "fs"),
        P(),
        P("fs", "tp"),
        P("fs", "tp"),
        P("tp"),
        P("tp"),
        P("tp", "fs"),
        P(None, "fs"),
    )
    dims = (mesh.shape["fs"], mesh.shape["tp"])
    return jax.shard_map(
        functools.partial(local, dims),
        mesh=mesh,
        in_specs=placed,
        out_specs=P(("grp", "fs"), "tp"),
        check_vma=False,
    )
```
